512 devices in a mesh: dp: 4 (over x), kv: 64 (over z, y), tp: 2 (over core).
Axes of the slice: x: 4, y: 8, z: 8, core: 2. Of those that a mesh axis runs over, the one named last changes fastest.
Arguments:
- tokens: bfloat16 [192, 2048], P(('dp', 'tp'), 'kv'), may hold values from -8 to 8
- mix_gain: float32 [2048], replicated, may hold values from 0.1 to 1.9
- w_gate: bfloat16 [2048, 4096], P(None, 'kv'), may hold values from -0.125 to 0.125
- w_value: bfloat16 [2048, 4096], P(None, 'kv'), may hold values from -0.125 to 0.125
- w_maps: bfloat16 [2048, 16384], P(None, 'kv'), may hold values from -0.125 to 0.125
- w_step: bfloat16 [2048, 64], replicated, may hold values from -0.125 to 0.125
- conv_value: float32 [4, 4096], P(None, 'kv'), may hold values from -0.5 to 0.5
- conv_maps: float32 [4, 16384], P(None, 'kv'), may hold values from -0.5 to 0.5
- past_value: bfloat16 [192, 3, 4096], P(('dp', 'tp'), None, 'kv'), may hold values from -6 to 6
- past_maps: bfloat16 [192, 3, 16384], P(('dp', 'tp'), None, 'kv'), may hold values from -6 to 6
- step_bias: float32 [64], P('kv'), may hold values from -3 to 0
- decay_log: float32 [64], P('kv'), may hold values from 0 to 2.77
- skip_gain: float32 [64], P('kv'), may hold values from 0.1 to 1.9
- head_gain: float32 [4096], P('kv'), may hold values from 0.1 to 1.9
- state: float32 [192, 64, 64, 128], P(('dp', 'tp'), 'kv'), may hold values from -2 to 2
- w_out: bfloat16 [4096, 2048], P('kv'), may hold values from -0.25 to 0.25
- mlp_gain: float32 [2048], replicated, may hold values from 0.1 to 1.9
- w_up: bfloat16 [2048, 8192], P(None, 'kv'), may hold values from -0.125 to 0.125
- w_down: bfloat16 [8192, 2048], P('kv'), may hold values from -0.1875 to 0.1875
Outputs:
- layer_out: bfloat16 [192, 2048], P(('dp', 'tp'), 'kv')
- state_next: float32 [192, 64, 64, 128], P(('dp', 'tp'), 'kv')
- value_tail: bfloat16 [192, 3, 4096], P(('dp', 'tp'), None, 'kv')
- maps_tail: bfloat16 [192, 3, 16384], P(('dp', 'tp'), None, 'kv')
The draws below stay inside these ranges and needn't reach their ends.
All inputs are finite; a program needn't handle non-finite values.
Results may differ from the reference program's by a relative error of at most 0.0081.
Values may be sent and summed in bfloat16 or wider, within the bound.
A program may use at most 64 MiB of HBM per device.

```python
import jax
import jax.numpy as jnp
from jax import lax

D = 2048
HEADS = 64
HEAD_DIM = 64
STATE = 128
GROUPS = 64
KERNEL = 4
FF = 8192
INNER = 4096
MAPS = 16384
BATCH = 192


def draw_tokens(key, part):
    streams = jax.random.split(jax.random.fold_in(key, 17), 4)
    columns = jnp.arange(D, dtype=jnp.float32)
    spread = jnp.exp(jax.random.uniform(streams[0], (D,), jnp.float32) * jnp.log(10.0))
    col_scale = spread * (1.0 + 3.0 * columns / D)
    col_scale = col_scale / jnp.sqrt(jnp.mean(col_scale * col_scale))
    noise_part = jax.random.normal(streams[1], (BATCH, D), jnp.float32)
    row_scale = jnp.exp(jax.random.uniform(streams[3], (BATCH, 1), jnp.float32, -0.35, 0.35))
    return jnp.clip(noise_part * col_scale[None, :] * row_scale, -8.0, 8.0).astype(jnp.bfloat16)


def with_spikes(result, stream_key, source, target, shards_of, factor):
    def block_of(position):
        return (jnp.arange(result.shape[position]) // (result.shape[position] // shards_of)).reshape((-1,) + (1,) * (result.ndim - 1 - position))

    near = jax.random.permutation(stream_key, shards_of)[block_of(target)]
    far = (block_of(target) + shards_of // 2) % shards_of
    return jnp.where((block_of(source) == near) | (block_of(source) == far), factor * result, result)


def block_levels(own_key, extent, cuts, least, largest):
    def one(position, shards_of):
        heights = jax.random.uniform(jax.random.fold_in(jax.random.fold_in(own_key, 6), position), (shards_of,), jnp.float32, least / len(cuts), largest / len(cuts))
        return jnp.repeat(jnp.exp(heights), extent[position] // shards_of).reshape((-1,) + (1,) * (len(extent) - position - 1))

    level = one(*cuts[0])
    for cut in cuts[1:]:
        level = level * one(*cut)
    return level


def noise(own_key, shape, scale, bound, cuts=(), kind=jnp.bfloat16):
    entries = jax.random.normal(own_key, shape, jnp.float32) * scale
    if len(cuts) > 0:
        entries = block_levels(own_key, shape, cuts, -0.22, 0.18) * entries
    return jnp.clip(entries, min=-bound, max=bound).astype(kind)


def heavy_noise(own_key, shape, deviation, limit, cuts, heavy, kind=jnp.bfloat16):
    entries = deviation * jax.random.normal(own_key, shape, jnp.float32)
    if cuts:
        entries = entries * block_levels(own_key, shape, cuts, -0.22, 0.18)
    return jnp.clip(with_spikes(entries, jax.random.fold_in(own_key, 3), *heavy), -limit, limit).astype(kind)


def setup_inputs(seed: int = 0) -> dict:
    streams_of = jax.random.split(jax.random.key(seed), 20)
    return {
        "tokens": draw_tokens(jax.random.fold_in(streams_of[19], 71), 0),
        "mix_gain": jnp.clip(1.0 + 0.18 * jax.random.normal(streams_of[1], (D,), jnp.float32), 0.1, 1.9),
        "w_gate": noise(streams_of[2], (D, INNER), D ** -0.5, 0.125, ((1, 64),)),
        "w_value": noise(streams_of[3], (D, INNER), D ** -0.5, 0.125, ((1, 64),)),
        "w_maps": noise(streams_of[4], (D, MAPS), D ** -0.5, 0.125, ((1, 64),)),
        "w_step": noise(streams_of[5], (D, HEADS), D ** -0.5, 0.125),
        "conv_value": jnp.clip(jax.random.uniform(streams_of[6], (KERNEL, INNER), jnp.float32, -0.5, 0.5) * block_levels(streams_of[6], (KERNEL, INNER), ((1, 64),), -0.4, 0.0), -0.5, 0.5),
        "conv_maps": jnp.clip(jax.random.uniform(streams_of[7], (KERNEL, MAPS), jnp.float32, -0.5, 0.5) * block_levels(streams_of[7], (KERNEL, MAPS), ((1, 64),), -0.4, 0.0), -0.5, 0.5),
        "past_value": noise(streams_of[8], (BATCH, KERNEL - 1, INNER), 1.0, 6.0, ((0, 8), (2, 64))),
        "past_maps": noise(streams_of[9], (BATCH, KERNEL - 1, MAPS), 1.0, 6.0, ((0, 8), (2, 64))),
        "step_bias": jnp.clip(-3.0 + 3.0 * jax.random.uniform(streams_of[10], (HEADS,), jnp.float32) ** block_levels(streams_of[10], (HEADS,), ((0, 64),), -0.2, 0.2), -3.0, 0.0),
        "decay_log": jnp.clip(2.77 * jax.random.uniform(streams_of[11], (HEADS,), jnp.float32) ** block_levels(streams_of[11], (HEADS,), ((0, 64),), -0.2, 0.2), 0.0, 2.77),
        "skip_gain": jnp.clip(1.0 + 0.18 * jax.random.normal(streams_of[12], (HEADS,), jnp.float32), 0.1, 1.9),
        "head_gain": jnp.clip(1.0 + 0.18 * jax.random.normal(streams_of[13], (INNER,), jnp.float32), 0.1, 1.9),
        "state": noise(streams_of[14], (BATCH, HEADS, HEAD_DIM, STATE), 0.3, 2.0, ((0, 8), (1, 64)), jnp.float32),
        "w_out": heavy_noise(streams_of[15], (INNER, D), INNER ** -0.5, 0.25, ((0, 64),), (0, 1, 64, 4.0)),
        "mlp_gain": jnp.clip(1.0 + 0.18 * jax.random.normal(streams_of[16], (D,), jnp.float32), 0.1, 1.9),
        "w_up": noise(streams_of[17], (D, FF), D ** -0.5, 0.125, ((1, 64),)),
        "w_down": heavy_noise(streams_of[18], (FF, D), FF ** -0.5, 0.1875, ((0, 64),), (0, 1, 64, 4.0)),
    }


NORM_EPS = 1e-05

def rms_rows(matrix, gain_vec):
    widened = matrix.astype(jnp.float32)
    inv_scale = lax.rsqrt(lax.optimization_barrier(jnp.mean(widened * widened, axis=-1, keepdims=True)) + NORM_EPS)
    return (widened * inv_scale * gain_vec).astype(jnp.bfloat16)

def short_conv(past_rows, newest, kernel):
    window = jnp.concatenate([past_rows, newest[:, None, :]], axis=1)
    summed = lax.optimization_barrier(jnp.sum(window.astype(jnp.float32) * kernel[None], axis=1))
    return (jax.nn.silu(summed), window[:, 1:, :])

def reference(tokens, mix_gain, w_gate, w_value, w_maps, w_step, conv_value, conv_maps, past_value, past_maps, step_bias, decay_log, skip_gain, head_gain, state, w_out, mlp_gain, w_up, w_down):
    normed = rms_rows(tokens, mix_gain)
    gate_pre = jnp.dot(normed, w_gate, preferred_element_type=jnp.float32)
    step_pre = jnp.dot(normed, w_step, preferred_element_type=jnp.float32)
    value_new = jnp.dot(normed, w_value, preferred_element_type=jnp.float32).astype(jnp.bfloat16)
    maps_new = jnp.dot(normed, w_maps, preferred_element_type=jnp.float32).astype(jnp.bfloat16)
    value_act, value_tail = short_conv(past_value, value_new, conv_value)
    maps_act, maps_tail = short_conv(past_maps, maps_new, conv_maps)
    rounded = lax.optimization_barrier(maps_act.astype(jnp.bfloat16))
    grouped = rounded.astype(jnp.float32).reshape(BATCH, GROUPS, 2, STATE)
    per_group = HEADS // GROUPS
    in_map = jnp.repeat(grouped[:, :, 0], per_group, axis=1)
    out_map = jnp.repeat(grouped[:, :, 1], per_group, axis=1)
    head_values = value_act.reshape(BATCH, HEADS, HEAD_DIM)
    step_size = jax.nn.softplus(step_pre + step_bias)
    decay_rate = jnp.exp(-step_size * jnp.exp(decay_log))
    written = (step_size[:, :, None] * head_values)[:, :, :, None] * in_map[:, :, None, :]
    state_next = decay_rate[:, :, None, None] * state + written
    read_out = lax.optimization_barrier(jnp.sum(state_next * out_map[:, :, None, :], axis=-1)) + skip_gain[None, :, None] * head_values
    gated_heads = read_out * jax.nn.silu(gate_pre.reshape(BATCH, HEADS, HEAD_DIM))
    inv_scale = lax.rsqrt(lax.optimization_barrier(jnp.mean(gated_heads * gated_heads, axis=-1, keepdims=True)) + NORM_EPS)
    heads_out = (gated_heads * inv_scale * head_gain.reshape(HEADS, HEAD_DIM)).reshape(BATCH, INNER)
    heads_out = heads_out.astype(jnp.bfloat16)
    mixer_out = jnp.dot(heads_out, w_out, preferred_element_type=jnp.float32)
    hidden = lax.optimization_barrier((tokens.astype(jnp.float32) + mixer_out).astype(jnp.bfloat16))
    normed_mlp = rms_rows(hidden, mlp_gain)
    squared = jnp.square(jax.nn.relu(jnp.dot(normed_mlp, w_up, preferred_element_type=jnp.float32)))
    squared = squared.astype(jnp.bfloat16)
    layer_out = hidden.astype(jnp.float32) + jnp.dot(squared, w_down, preferred_element_type=jnp.float32)
    return (layer_out.astype(jnp.bfloat16), state_next, value_tail, maps_tail)
```

```python
import jax
import jax.numpy as jnp
from jax import lax
from jax.experimental import pallas as pl
from jax.experimental.pallas import tpu as pltpu
from jax.sharding import PartitionSpec as P

F32 = jnp.float32
BF16 = jnp.bfloat16
NORM_EPS = 1e-05
SIDE = 8
NEAR = (1, 7, 2, 6, 3, 5, 4)
FAR = (4, 3, 5, 2, 6, 1, 7)
MESH = pl.DeviceIdType.MESH
NAMES = (
    "tokens",
    "mix_gain",
    "w_gate",
    "w_value",
    "w_maps",
    "w_step",
    "conv_value",
    "conv_maps",
    "past_value",
    "past_maps",
    "step_bias",
    "decay_log",
    "skip_gain",
    "head_gain",
    "state",
    "w_out",
    "mlp_gain",
    "w_up",
    "w_down",
)
ORDER = (
    "mix_gain",
    "w_maps",
    "w_gate",
    "w_value",
    "w_step",
    "past_value",
    "past_maps",
    "conv_value",
    "conv_maps",
    "step_bias",
    "decay_log",
    "skip_gain",
    "head_gain",
    "state",
    "w_out",
    "mlp_gain",
    "w_up",
    "w_down",
)


def silu(v):
    return v * (1.0 / (1.0 + jnp.exp(-v)))


def softplus(v):
    return jnp.maximum(v, 0.0) + jnp.log1p(jnp.exp(-jnp.abs(v)))


def dot(a, b):
    return lax.dot_general(a, b, (((1,), (0,)), ((), ())), preferred_element_type=F32)


def dot_t(a, b):
    return lax.dot_general(a, b, (((1,), (1,)), ((), ())), preferred_element_type=F32)


def kernel(*refs):
    n_in = len(NAMES)
    hbm = dict(zip(NAMES, refs[:n_in]))
    layer_out, state_next, value_tail, maps_tail = refs[n_in : n_in + 4]
    vm = dict(zip(NAMES, refs[n_in + 4 : 2 * n_in + 4]))
    (
        snext_buf, xbuf, xs, pbuf, r1, r2, hbuf, fbuf, f1, fpk, f2,
        load_sem, store_sem, a_s, a_r, s1, q1, s2, q2, s3, q3, s4, q4, s5, q5,
    ) = refs[2 * n_in + 4 :]

    me = lax.axis_index("kv")
    z = me // SIDE
    y = lax.rem(me, SIDE)

    def zpeer(d):
        return {"kv": lax.rem(z + d, SIDE) * SIDE + y}

    def ypeer(d):
        return {"kv": z * SIDE + lax.rem(y + d, SIDE)}

    def zsrc(d):
        return lax.rem(z + SIDE - d, SIDE)

    def ysrc(d):
        return lax.rem(y + SIDE - d, SIDE)

    def load(name):
        src = hbm[name]
        if name == "w_step":
            src = src.at[pl.ds(pl.multiple_of(z * SIDE, SIDE), SIDE), :]
        return pltpu.make_async_copy(src, vm[name], load_sem.at[NAMES.index(name)])

    sent = []

    def send(src, dst, ssem, rsem, peer):
        copy = pltpu.make_async_remote_copy(
            src_ref=src, dst_ref=dst, send_sem=ssem, recv_sem=rsem, device_id=peer, device_id_type=MESH
        )
        copy.start()
        sent.append(copy)

    def arrived(dst, ssem, rsem):
        pltpu.make_async_remote_copy(
            src_ref=dst, dst_ref=dst, send_sem=ssem, recv_sem=rsem, device_id=zpeer(1), device_id_type=MESH
        ).wait_recv()

    load("tokens").start()
    barrier = pltpu.get_barrier_semaphore()
    for d in FAR:
        pl.semaphore_signal(barrier, inc=1, device_id=zpeer(d), device_id_type=MESH)
        pl.semaphore_signal(barrier, inc=1, device_id=ypeer(d), device_id_type=MESH)
    for name in ORDER:
        load(name).start()

    lane = lax.broadcasted_iota(jnp.int32, (8, 128), 1)

    load("tokens").wait()
    own = vm["tokens"][...].astype(F32)
    packed = jnp.concatenate([own[0:8], own[8:16], own[16:24], jnp.zeros((8, 32), F32)], axis=1)
    xbuf[z, y] = packed.astype(BF16)
    pl.semaphore_wait(barrier, 14)
    for d in FAR:
        send(xbuf.at[z, y], xbuf.at[z, y], a_s.at[0, d], a_r.at[0, d], ypeer(d))
        send(xbuf.at[z, y], xbuf.at[z, y], a_s.at[d, 0], a_r.at[d, 0], zpeer(d))

    for name in ORDER[:11]:
        load(name).wait()
    conv_v = vm["conv_value"][...]
    conv_m = vm["conv_maps"][...]
    pre_v = sum(vm["past_value"][k].astype(F32) * conv_v[k : k + 1] for k in range(3))
    pre_m = sum(vm["past_maps"][k].astype(F32) * conv_m[k : k + 1] for k in range(3))
    for k in range(2):
        value_tail[k] = vm["past_value"][k + 1]
        maps_tail[k] = vm["past_maps"][k + 1]

    for dy in NEAR:
        block = xbuf.at[z, ysrc(dy)]
        arrived(block, a_s.at[0, dy], a_r.at[0, dy])
        for d in FAR:
            send(block, block, a_s.at[d, dy], a_r.at[d, dy], zpeer(d))

    sq = jnp.zeros((24, 128), F32)
    acc_g = jnp.zeros((24, 64), F32)
    acc_v = jnp.zeros((24, 64), F32)
    acc_s = jnp.zeros((24, 8), F32)
    acc_m = jnp.zeros((24, 256), F32)
    for dz in (0,) + NEAR:
        zi = zsrc(dz)
        if dz:
            for dy in range(SIDE):
                arrived(xbuf.at[zi, ysrc(dy)], a_s.at[dz, dy], a_r.at[dz, dy])
        halves = []
        for t in range(2):
            parts = []
            blocks = [xbuf[zi, 4 * t + j].astype(F32) for j in range(4)]
            for g in range(3):
                tile = None
                for j in range(4):
                    shift = (32 * j - 32 * g) % 128
                    moved = pltpu.roll(blocks[j], shift, 1) if shift else blocks[j]
                    tile = moved if tile is None else jnp.where(lane >= 32 * j, moved, tile)
                parts.append(tile)
            tile = jnp.concatenate(parts, axis=0)
            xs[2 * zi + t] = tile
            sq = sq + tile * tile
            halves.append((tile * vm["mix_gain"][pl.ds(2 * zi + t, 1), :]).astype(BF16))
        lhs = jnp.concatenate(halves, axis=1)
        cols = pl.ds(pl.multiple_of(zi * 256, 256), 256)
        acc_m = acc_m + dot(lhs, vm["w_maps"][cols, :])
        acc_g = acc_g + dot_t(lhs, vm["w_gate"][:, cols])
        acc_v = acc_v + dot_t(lhs, vm["w_value"][:, cols])
        acc_s = acc_s + dot_t(lhs, vm["w_step"][:, cols])

    inv = lax.rsqrt(jnp.sum(sq, axis=1, keepdims=True) * (1.0 / 2048.0) + NORM_EPS)
    gate_pre = acc_g * inv
    value_new = (acc_v * inv).astype(BF16)
    maps_new = (acc_m * inv).astype(BF16)
    value_tail[2] = value_new
    maps_tail[2] = maps_new
    step_lane = lax.broadcasted_iota(jnp.int32, (24, 8), 1)
    step_pre = jnp.sum(jnp.where(step_lane == y, acc_s, 0.0), axis=1, keepdims=True) * inv

    value_act = silu(pre_v + value_new.astype(F32) * conv_v[3:4])
    maps_act = silu(pre_m + maps_new.astype(F32) * conv_m[3:4]).astype(BF16).astype(F32)
    in_map = maps_act[:, :128]
    out_map = maps_act[:, 128:]
    step_size = softplus(step_pre + vm["step_bias"][...])
    decay = jnp.exp(-step_size * jnp.exp(vm["decay_log"][...]))

    load("state").wait()
    lane64 = lax.broadcasted_iota(jnp.int32, (64, 128), 1)
    reads = jnp.zeros((64, 128), F32)
    for b in range(24):
        total = jnp.sum(vm["state"][b] * out_map[b : b + 1, :], axis=1, keepdims=True)
        reads = jnp.where(lane64 == b, total, reads)
    old_read = jnp.transpose(jnp.concatenate([reads, jnp.zeros((64, 128), F32)], axis=0))[:24, :64]
    met = jnp.sum(in_map * out_map, axis=1, keepdims=True)
    load("skip_gain").wait()
    load("head_gain").wait()
    written = step_size * value_act
    read_out = decay * old_read + written * met + vm["skip_gain"][...] * value_act
    gated = read_out * silu(gate_pre)
    head_inv = lax.rsqrt(jnp.sum(gated * gated, axis=1, keepdims=True) * (1.0 / 64.0) + NORM_EPS)
    heads_out = (gated * head_inv * vm["head_gain"][...]).astype(BF16)

    load("w_out").wait()
    for c in range(16):
        pbuf[c] = dot(heads_out, vm["w_out"][:, c * 128 : c * 128 + 128]).astype(BF16)

    for d in FAR:
        send(pbuf.at[lax.rem(z + d, SIDE)], r1.at[0, d], s1.at[0, d], q1.at[0, d], zpeer(d))
        send(pbuf.at[8 + lax.rem(y + d, SIDE)], r1.at[1, d], s1.at[1, d], q1.at[1, d], ypeer(d))

    decay_rows = jnp.broadcast_to(decay, (24, 128))
    padded = jnp.concatenate([written, jnp.zeros((24, 64), F32)], axis=1)
    padded = jnp.concatenate([padded, jnp.zeros((104, 128), F32)], axis=0)
    columns = jnp.transpose(padded)[:64, :]
    for b in range(24):
        snext_buf[b] = (
            decay_rows[b : b + 1, :] * vm["state"][b] + columns[:, b : b + 1] * in_map[b : b + 1, :]
        )
    state_out = pltpu.make_async_copy(snext_buf, state_next, store_sem)
    state_out.start()
    for name in ORDER[-3:]:
        load(name).wait()

    sum_p = pbuf[z].astype(F32)
    sum_q = pbuf[8 + y].astype(F32)
    for d in NEAR:
        arrived(r1.at[0, d], s1.at[0, d], q1.at[0, d])
        sum_p = sum_p + r1[0, d].astype(F32)
        arrived(r1.at[1, d], s1.at[1, d], q1.at[1, d])
        sum_q = sum_q + r1[1, d].astype(F32)
    r2[0, y] = sum_p.astype(BF16)
    r2[1, z] = sum_q.astype(BF16)
    for d in FAR:
        send(r2.at[0, y], r2.at[0, y], s2.at[0, d], q2.at[0, d], ypeer(d))
        send(r2.at[1, z], r2.at[1, z], s2.at[1, d], q2.at[1, d], zpeer(d))
    for d in NEAR:
        arrived(r2.at[0, ysrc(d)], s2.at[0, d], q2.at[0, d])
        arrived(r2.at[1, zsrc(d)], s2.at[1, d], q2.at[1, d])
    sum_p = r2[0, 0].astype(F32)
    sum_q = r2[1, 0].astype(F32)
    for k in range(1, SIDE):
        sum_p = sum_p + r2[0, k].astype(F32)
        sum_q = sum_q + r2[1, k].astype(F32)
    hbuf[z] = (xs[z] + sum_p).astype(BF16)
    hbuf[8 + y] = (xs[8 + y] + sum_q).astype(BF16)
    for d in FAR:
        send(hbuf.at[z], hbuf.at[z], s3.at[0, d], q3.at[0, d], zpeer(d))
        send(hbuf.at[8 + y], hbuf.at[8 + y], s3.at[1, d], q3.at[1, d], ypeer(d))

    sq = jnp.zeros((24, 128), F32)
    up = jnp.zeros((24, 128), F32)
    for d in (0,) + NEAR:
        for half in range(2):
            c = zsrc(d) if half == 0 else 8 + ysrc(d)
            if d:
                arrived(hbuf.at[c], s3.at[half, d], q3.at[half, d])
            h = hbuf[c].astype(F32)
            sq = sq + h * h
            scaled = (h * vm["mlp_gain"][pl.ds(c, 1), :]).astype(BF16)
            up = up + dot(scaled, vm["w_up"][pl.ds(pl.multiple_of(c * 128, 128), 128), :])
    inv = lax.rsqrt(jnp.sum(sq, axis=1, keepdims=True) * (1.0 / 2048.0) + NORM_EPS)
    relu = jnp.maximum(up * inv, 0.0)
    squared = (relu * relu).astype(BF16)
    for c in range(16):
        fbuf[c // 2, c % 2] = dot(squared, vm["w_down"][:, c * 128 : c * 128 + 128]).astype(BF16)

    for d in FAR:
        send(fbuf.at[lax.rem(z + d, SIDE)], f1.at[d], s4.at[d], q4.at[d], zpeer(d))
    total = fbuf[z].astype(F32)
    for d in NEAR:
        arrived(f1.at[d], s4.at[d], q4.at[d])
        total = total + f1[d].astype(F32)
    for t in range(2):
        for j in range(4):
            tile = None
            for g in range(3):
                shift = (32 * g - 32 * j) % 128
                rows = total[t, 8 * g : 8 * g + 8, :]
                moved = pltpu.roll(rows, shift, 1) if shift else rows
                tile = moved if tile is None else jnp.where(lane >= 32 * g, moved, tile)
            fpk[4 * t + j] = tile.astype(BF16)
    for d in FAR:
        send(fpk.at[lax.rem(y + d, SIDE)], f2.at[d], s5.at[d], q5.at[d], ypeer(d))
    total = fpk[y].astype(F32)
    for d in NEAR:
        arrived(f2.at[d], s5.at[d], q5.at[d])
        total = total + f2[d].astype(F32)
    mlp = jnp.concatenate(
        [total[:, :32], pltpu.roll(total, 96, 1)[:, :32], pltpu.roll(total, 64, 1)[:, :32]], axis=0
    )
    near_cols = hbuf[2 * z + y // 4].astype(F32)
    own_hidden = pltpu.roll(near_cols, lax.rem(128 - 32 * lax.rem(y, 4), 128), 1)[:, :32]
    layer_out[...] = (own_hidden + mlp).astype(BF16)

    for copy in sent:
        copy.wait_send()
    state_out.wait()


def local(
    tokens, mix_gain, w_gate, w_value, w_maps, w_step, conv_value, conv_maps, past_value, past_maps,
    step_bias, decay_log, skip_gain, head_gain, state, w_out, mlp_gain, w_up, w_down,
):
    args = (
        tokens,
        mix_gain.reshape(16, 128),
        w_gate.T,
        w_value.T,
        w_maps,
        w_step.T,
        conv_value,
        conv_maps,
        jnp.transpose(past_value, (1, 0, 2)),
        jnp.transpose(past_maps, (1, 0, 2)),
        step_bias.reshape(1, 1),
        decay_log.reshape(1, 1),
        skip_gain.reshape(1, 1),
        head_gain.reshape(1, 64),
        state.reshape(24, 64, 128),
        w_out,
        mlp_gain.reshape(16, 128),
        w_up,
        w_down,
    )
    buffers = []
    for k, a in enumerate(args):
        shape = (SIDE, 2048) if k == 5 else a.shape
        buffers.append(pltpu.VMEM(shape, a.dtype))
    dma = pltpu.SemaphoreType.DMA
    layer_out, state_next, value_tail, maps_tail = pl.pallas_call(
        kernel,
        out_shape=(
            jax.ShapeDtypeStruct((24, 32), BF16),
            jax.ShapeDtypeStruct((24, 64, 128), F32),
            jax.ShapeDtypeStruct((3, 24, 64), BF16),
            jax.ShapeDtypeStruct((3, 24, 256), BF16),
        ),
        in_specs=[pl.BlockSpec(memory_space=pltpu.HBM)] * len(args),
        out_specs=(
            pl.BlockSpec(memory_space=pltpu.VMEM),
            pl.BlockSpec(memory_space=pltpu.HBM),
            pl.BlockSpec(memory_space=pltpu.VMEM),
            pl.BlockSpec(memory_space=pltpu.VMEM),
        ),
        scratch_shapes=buffers
        + [
            pltpu.VMEM((24, 64, 128), F32),
            pltpu.VMEM((SIDE, SIDE, 8, 128), BF16),
            pltpu.VMEM((16, 24, 128), F32),
            pltpu.VMEM((16, 24, 128), BF16),
            pltpu.VMEM((2, SIDE, 24, 128), BF16),
            pltpu.VMEM((2, SIDE, 24, 128), BF16),
            pltpu.VMEM((16, 24, 128), BF16),
            pltpu.VMEM((SIDE, 2, 24, 128), BF16),
            pltpu.VMEM((SIDE, 2, 24, 128), BF16),
            pltpu.VMEM((SIDE, 8, 128), BF16),
            pltpu.VMEM((SIDE, 8, 128), BF16),
            dma((len(args),)),
            dma,
            dma((SIDE, SIDE)),
            dma((SIDE, SIDE)),
            dma((2, SIDE)),
            dma((2, SIDE)),
            dma((2, SIDE)),
            dma((2, SIDE)),
            dma((2, SIDE)),
            dma((2, SIDE)),
            dma((SIDE,)),
            dma((SIDE,)),
            dma((SIDE,)),
            dma((SIDE,)),
        ],
        compiler_params=pltpu.CompilerParams(collective_id=0, has_side_effects=True, vmem_limit_bytes=67043328),
        name="layer",
    )(*args)
    return (
        layer_out,
        state_next.reshape(24, 1, 64, 128),
        jnp.transpose(value_tail, (1, 0, 2)),
        jnp.transpose(maps_tail, (1, 0, 2)),
    )


def solution(mesh):
    rows = ("dp", "tp")
    in_specs = (
        P(rows, "kv"),
        P(),
        P(None, "kv"),
        P(None, "kv"),
        P(None, "kv"),
        P(),
        P(None, "kv"),
        P(None, "kv"),
        P(rows, None, "kv"),
        P(rows, None, "kv"),
        P("kv"),
        P("kv"),
        P("kv"),
        P("kv"),
        P(rows, "kv", None, None),
        P("kv", None),
        P(),
        P(None, "kv"),
        P("kv", None),
    )
    out_specs = (
        P(rows, "kv"),
        P(rows, "kv", None, None),
        P(rows, None, "kv"),
        P(rows, None, "kv"),
    )
    return jax.shard_map(local, mesh=mesh, in_specs=in_specs, out_specs=out_specs, check_vma=False)
```

```python
import jax
import jax.numpy as jnp
from jax import lax
from jax.experimental import pallas as pl
from jax.experimental.pallas import tpu as pltpu
from jax.sharding import PartitionSpec as P

F32 = jnp.float32
BF16 = jnp.bfloat16
NORM_EPS = 1e-05
SIDE = 8
NEAR = (1, 7, 2, 6, 3, 5, 4)
FAR = (4, 3, 5, 2, 6, 1, 7)
MESH = pl.DeviceIdType.MESH
NAMES = (
    "tokens",
    "mix_gain",
    "w_gate",
    "w_value",
    "w_maps",
    "w_step",
    "conv_value",
    "conv_maps",
    "past_value",
    "past_maps",
    "step_bias",
    "decay_log",
    "skip_gain",
    "head_gain",
    "state",
    "w_out",
    "mlp_gain",
    "w_up",
    "w_down",
)
ORDER = (
    "mix_gain",
    "w_maps",
    "w_gate",
    "w_value",
    "w_step",
    "past_value",
    "past_maps",
    "conv_value",
    "conv_maps",
    "step_bias",
    "decay_log",
    "skip_gain",
    "head_gain",
    "state",
    "w_out",
    "mlp_gain",
    "w_up",
    "w_down",
)


def silu(v):
    return v * (1.0 / (1.0 + jnp.exp(-v)))


def softplus(v):
    return jnp.maximum(v, 0.0) + jnp.log1p(jnp.exp(-jnp.abs(v)))


def dot(a, b):
    return lax.dot_general(a, b, (((1,), (0,)), ((), ())), preferred_element_type=F32)


def dot_t(a, b):
    return lax.dot_general(a, b, (((1,), (1,)), ((), ())), preferred_element_type=F32)


def kernel(*refs):
    n_in = len(NAMES)
    hbm = dict(zip(NAMES, refs[:n_in]))
    layer_out, state_next, value_tail, maps_tail = refs[n_in : n_in + 4]
    vm = dict(zip(NAMES, refs[n_in + 4 : 2 * n_in + 4]))
    (
        xbuf, xs, pbuf, r1, r2, hbuf, fbuf, f1, fpk, f2,
        load_sem, a_s, a_r, s1, q1, s2, q2, s3, q3, s4, q4, s5, q5,
    ) = refs[2 * n_in + 4 :]

    me = lax.axis_index("kv")
    z = me // SIDE
    y = lax.rem(me, SIDE)

    def zpeer(d):
        return {"kv": lax.rem(z + d, SIDE) * SIDE + y}

    def ypeer(d):
        return {"kv": z * SIDE + lax.rem(y + d, SIDE)}

    def zsrc(d):
        return lax.rem(z + SIDE - d, SIDE)

    def ysrc(d):
        return lax.rem(y + SIDE - d, SIDE)

    def load(name):
        src = hbm[name]
        if name == "w_step":
            src = src.at[pl.ds(pl.multiple_of(z * SIDE, SIDE), SIDE), :]
        return pltpu.make_async_copy(src, vm[name], load_sem.at[NAMES.index(name)])

    sent = []

    def send(src, dst, ssem, rsem, peer):
        copy = pltpu.make_async_remote_copy(
            src_ref=src, dst_ref=dst, send_sem=ssem, recv_sem=rsem, device_id=peer, device_id_type=MESH
        )
        copy.start()
        sent.append(copy)

    def arrived(dst, ssem, rsem):
        pltpu.make_async_remote_copy(
            src_ref=dst, dst_ref=dst, send_sem=ssem, recv_sem=rsem, device_id=zpeer(1), device_id_type=MESH
        ).wait_recv()

    load("tokens").start()
    barrier = pltpu.get_barrier_semaphore()
    for d in FAR:
        pl.semaphore_signal(barrier, inc=1, device_id=zpeer(d), device_id_type=MESH)
        pl.semaphore_signal(barrier, inc=1, device_id=ypeer(d), device_id_type=MESH)
    for name in ORDER:
        load(name).start()

    lane = lax.broadcasted_iota(jnp.int32, (8, 128), 1)

    load("tokens").wait()
    own = vm["tokens"][...].astype(F32)
    packed = jnp.concatenate([own[0:8], own[8:16], own[16:24], jnp.zeros((8, 32), F32)], axis=1)
    xbuf[z, y] = packed.astype(BF16)
    pl.semaphore_wait(barrier, 14)
    for d in FAR:
        send(xbuf.at[z, y], xbuf.at[z, y], a_s.at[0, d], a_r.at[0, d], ypeer(d))
        send(xbuf.at[z, y], xbuf.at[z, y], a_s.at[d, 0], a_r.at[d, 0], zpeer(d))

    for name in ORDER[:11]:
        load(name).wait()
    conv_v = vm["conv_value"][...]
    conv_m = vm["conv_maps"][...]
    pre_v = sum(vm["past_value"][k].astype(F32) * conv_v[k : k + 1] for k in range(3))
    pre_m = sum(vm["past_maps"][k].astype(F32) * conv_m[k : k + 1] for k in range(3))
    for k in range(2):
        value_tail[k] = vm["past_value"][k + 1]
        maps_tail[k] = vm["past_maps"][k + 1]

    for dy in NEAR:
        block = xbuf.at[z, ysrc(dy)]
        arrived(block, a_s.at[0, dy], a_r.at[0, dy])
        for d in FAR:
            send(block, block, a_s.at[d, dy], a_r.at[d, dy], zpeer(d))

    sq = jnp.zeros((24, 128), F32)
    acc_g = jnp.zeros((24, 64), F32)
    acc_v = jnp.zeros((24, 64), F32)
    acc_s = jnp.zeros((24, 8), F32)
    acc_m = jnp.zeros((24, 256), F32)
    for dz in (0,) + NEAR:
        zi = zsrc(dz)
        if dz:
            for dy in range(SIDE):
                arrived(xbuf.at[zi, ysrc(dy)], a_s.at[dz, dy], a_r.at[dz, dy])
        halves = []
        for t in range(2):
            parts = []
            blocks = [xbuf[zi, 4 * t + j].astype(F32) for j in range(4)]
            for g in range(3):
                tile = None
                for j in range(4):
                    shift = (32 * j - 32 * g) % 128
                    moved = pltpu.roll(blocks[j], shift, 1) if shift else blocks[j]
                    tile = moved if tile is None else jnp.where(lane >= 32 * j, moved, tile)
                parts.append(tile)
            tile = jnp.concatenate(parts, axis=0)
            xs[2 * zi + t] = tile
            sq = sq + tile * tile
            halves.append((tile * vm["mix_gain"][pl.ds(2 * zi + t, 1), :]).astype(BF16))
        lhs = jnp.concatenate(halves, axis=1)
        cols = pl.ds(pl.multiple_of(zi * 256, 256), 256)
        acc_m = acc_m + dot(lhs, vm["w_maps"][cols, :])
        acc_g = acc_g + dot_t(lhs, vm["w_gate"][:, cols])
        acc_v = acc_v + dot_t(lhs, vm["w_value"][:, cols])
        acc_s = acc_s + dot_t(lhs, vm["w_step"][:, cols])

    inv = lax.rsqrt(jnp.sum(sq, axis=1, keepdims=True) * (1.0 / 2048.0) + NORM_EPS)
    gate_pre = acc_g * inv
    value_new = (acc_v * inv).astype(BF16)
    maps_new = (acc_m * inv).astype(BF16)
    value_tail[2] = value_new
    maps_tail[2] = maps_new
    step_lane = lax.broadcasted_iota(jnp.int32, (24, 8), 1)
    step_pre = jnp.sum(jnp.where(step_lane == y, acc_s, 0.0), axis=1, keepdims=True) * inv

    value_act = silu(pre_v + value_new.astype(F32) * conv_v[3:4])
    maps_act = silu(pre_m + maps_new.astype(F32) * conv_m[3:4]).astype(BF16).astype(F32)
    in_map = maps_act[:, :128]
    out_map = maps_act[:, 128:]
    step_size = softplus(step_pre + vm["step_bias"][...])
    decay = jnp.exp(-step_size * jnp.exp(vm["decay_log"][...]))

    load("state").wait()
    lane64 = lax.broadcasted_iota(jnp.int32, (64, 128), 1)
    reads = jnp.zeros((64, 128), F32)
    for b in range(24):
        total = jnp.sum(vm["state"][b] * out_map[b : b + 1, :], axis=1, keepdims=True)
        reads = jnp.where(lane64 == b, total, reads)
    old_read = jnp.transpose(jnp.concatenate([reads, jnp.zeros((64, 128), F32)], axis=0))[:24, :64]
    met = jnp.sum(in_map * out_map, axis=1, keepdims=True)
    load("skip_gain").wait()
    load("head_gain").wait()
    written = step_size * value_act
    read_out = decay * old_read + written * met + vm["skip_gain"][...] * value_act
    gated = read_out * silu(gate_pre)
    head_inv = lax.rsqrt(jnp.sum(gated * gated, axis=1, keepdims=True) * (1.0 / 64.0) + NORM_EPS)
    heads_out = (gated * head_inv * vm["head_gain"][...]).astype(BF16)

    load("w_out").wait()
    for c in range(16):
        pbuf[c] = dot(heads_out, vm["w_out"][:, c * 128 : c * 128 + 128]).astype(BF16)

    for d in FAR:
        send(pbuf.at[lax.rem(z + d, SIDE)], r1.at[0, d], s1.at[0, d], q1.at[0, d], zpeer(d))
        send(pbuf.at[8 + lax.rem(y + d, SIDE)], r1.at[1, d], s1.at[1, d], q1.at[1, d], ypeer(d))

    decay_rows = jnp.broadcast_to(decay, (24, 128))
    padded = jnp.concatenate([written, jnp.zeros((24, 64), F32)], axis=1)
    padded = jnp.concatenate([padded, jnp.zeros((104, 128), F32)], axis=0)
    columns = jnp.transpose(padded)[:64, :]
    for b in range(24):
        state_next[b] = (
            decay_rows[b : b + 1, :] * vm["state"][b] + columns[:, b : b + 1] * in_map[b : b + 1, :]
        )
    for name in ORDER[-3:]:
        load(name).wait()

    sum_p = pbuf[z].astype(F32)
    sum_q = pbuf[8 + y].astype(F32)
    for d in NEAR:
        arrived(r1.at[0, d], s1.at[0, d], q1.at[0, d])
        sum_p = sum_p + r1[0, d].astype(F32)
        arrived(r1.at[1, d], s1.at[1, d], q1.at[1, d])
        sum_q = sum_q + r1[1, d].astype(F32)
    r2[0, y] = sum_p.astype(BF16)
    r2[1, z] = sum_q.astype(BF16)
    for d in FAR:
        send(r2.at[0, y], r2.at[0, y], s2.at[0, d], q2.at[0, d], ypeer(d))
        send(r2.at[1, z], r2.at[1, z], s2.at[1, d], q2.at[1, d], zpeer(d))
    for d in NEAR:
        arrived(r2.at[0, ysrc(d)], s2.at[0, d], q2.at[0, d])
        arrived(r2.at[1, zsrc(d)], s2.at[1, d], q2.at[1, d])
    sum_p = r2[0, 0].astype(F32)
    sum_q = r2[1, 0].astype(F32)
    for k in range(1, SIDE):
        sum_p = sum_p + r2[0, k].astype(F32)
        sum_q = sum_q + r2[1, k].astype(F32)
    hbuf[z] = (xs[z] + sum_p).astype(BF16)
    hbuf[8 + y] = (xs[8 + y] + sum_q).astype(BF16)
    for d in FAR:
        send(hbuf.at[z], hbuf.at[z], s3.at[0, d], q3.at[0, d], zpeer(d))
        send(hbuf.at[8 + y], hbuf.at[8 + y], s3.at[1, d], q3.at[1, d], ypeer(d))

    sq = jnp.zeros((24, 128), F32)
    up = jnp.zeros((24, 128), F32)
    for d in (0,) + NEAR:
        for half in range(2):
            c = zsrc(d) if half == 0 else 8 + ysrc(d)
            if d:
                arrived(hbuf.at[c], s3.at[half, d], q3.at[half, d])
            h = hbuf[c].astype(F32)
            sq = sq + h * h
            scaled = (h * vm["mlp_gain"][pl.ds(c, 1), :]).astype(BF16)
            up = up + dot(scaled, vm["w_up"][pl.ds(pl.multiple_of(c * 128, 128), 128), :])
    inv = lax.rsqrt(jnp.sum(sq, axis=1, keepdims=True) * (1.0 / 2048.0) + NORM_EPS)
    relu = jnp.maximum(up * inv, 0.0)
    squared = (relu * relu).astype(BF16)
    for c in range(16):
        fbuf[c // 2, c % 2] = dot(squared, vm["w_down"][:, c * 128 : c * 128 + 128]).astype(BF16)

    for d in FAR:
        send(fbuf.at[lax.rem(z + d, SIDE)], f1.at[d], s4.at[d], q4.at[d], zpeer(d))
    total = fbuf[z].astype(F32)
    for d in NEAR:
        arrived(f1.at[d], s4.at[d], q4.at[d])
        total = total + f1[d].astype(F32)
    for t in range(2):
        for j in range(4):
            tile = None
            for g in range(3):
                shift = (32 * g - 32 * j) % 128
                rows = total[t, 8 * g : 8 * g + 8, :]
                moved = pltpu.roll(rows, shift, 1) if shift else rows
                tile = moved if tile is None else jnp.where(lane >= 32 * g, moved, tile)
            fpk[4 * t + j] = tile.astype(BF16)
    for d in FAR:
        send(fpk.at[lax.rem(y + d, SIDE)], f2.at[d], s5.at[d], q5.at[d], ypeer(d))
    total = fpk[y].astype(F32)
    for d in NEAR:
        arrived(f2.at[d], s5.at[d], q5.at[d])
        total = total + f2[d].astype(F32)
    mlp = jnp.concatenate(
        [total[:, :32], pltpu.roll(total, 96, 1)[:, :32], pltpu.roll(total, 64, 1)[:, :32]], axis=0
    )
    near_cols = hbuf[2 * z + y // 4].astype(F32)
    own_hidden = pltpu.roll(near_cols, lax.rem(128 - 32 * lax.rem(y, 4), 128), 1)[:, :32]
    layer_out[...] = (own_hidden + mlp).astype(BF16)

    for copy in sent:
        copy.wait_send()


def hand_over(*refs):
    copies = [pltpu.make_async_copy(refs[k], refs[4 + k], refs[8].at[k]) for k in range(4)]
    for copy in copies:
        copy.start()
    for copy in copies:
        copy.wait()


def local(
    tokens, mix_gain, w_gate, w_value, w_maps, w_step, conv_value, conv_maps, past_value, past_maps,
    step_bias, decay_log, skip_gain, head_gain, state, w_out, mlp_gain, w_up, w_down,
):
    args = (
        tokens,
        mix_gain.reshape(16, 128),
        w_gate.T,
        w_value.T,
        w_maps,
        w_step.T,
        conv_value,
        conv_maps,
        jnp.transpose(past_value, (1, 0, 2)),
        jnp.transpose(past_maps, (1, 0, 2)),
        step_bias.reshape(1, 1),
        decay_log.reshape(1, 1),
        skip_gain.reshape(1, 1),
        head_gain.reshape(1, 64),
        state.reshape(24, 64, 128),
        w_out,
        mlp_gain.reshape(16, 128),
        w_up,
        w_down,
    )
    buffers = []
    for k, a in enumerate(args):
        shape = (SIDE, 2048) if k == 5 else a.shape
        buffers.append(pltpu.VMEM(shape, a.dtype))
    dma = pltpu.SemaphoreType.DMA
    layer_out, state_next, value_tail, maps_tail = pl.pallas_call(
        kernel,
        out_shape=(
            jax.ShapeDtypeStruct((24, 32), BF16),
            jax.ShapeDtypeStruct((24, 64, 128), F32),
            jax.ShapeDtypeStruct((3, 24, 64), BF16),
            jax.ShapeDtypeStruct((3, 24, 256), BF16),
        ),
        in_specs=[pl.BlockSpec(memory_space=pltpu.HBM)] * len(args),
        out_specs=(
            pl.BlockSpec(memory_space=pltpu.VMEM),
            pl.BlockSpec(memory_space=pltpu.VMEM),
            pl.BlockSpec(memory_space=pltpu.VMEM),
            pl.BlockSpec(memory_space=pltpu.VMEM),
        ),
        scratch_shapes=buffers
        + [
            pltpu.VMEM((SIDE, SIDE, 8, 128), BF16),
            pltpu.VMEM((16, 24, 128), F32),
            pltpu.VMEM((16, 24, 128), BF16),
            pltpu.VMEM((2, SIDE, 24, 128), BF16),
            pltpu.VMEM((2, SIDE, 24, 128), BF16),
            pltpu.VMEM((16, 24, 128), BF16),
            pltpu.VMEM((SIDE, 2, 24, 128), BF16),
            pltpu.VMEM((SIDE, 2, 24, 128), BF16),
            pltpu.VMEM((SIDE, 8, 128), BF16),
            pltpu.VMEM((SIDE, 8, 128), BF16),
            dma((len(args),)),
            dma((SIDE, SIDE)),
            dma((SIDE, SIDE)),
            dma((2, SIDE)),
            dma((2, SIDE)),
            dma((2, SIDE)),
            dma((2, SIDE)),
            dma((2, SIDE)),
            dma((2, SIDE)),
            dma((SIDE,)),
            dma((SIDE,)),
            dma((SIDE,)),
            dma((SIDE,)),
        ],
        compiler_params=pltpu.CompilerParams(collective_id=0, has_side_effects=True, vmem_limit_bytes=48 * 2**20),
        name="layer",
    )(*[a if a.size == 1 else pltpu.with_memory_space_constraint(a, pltpu.HBM) for a in args])
    layer_out, state_next, value_tail, maps_tail = pl.pallas_call(
        hand_over,
        out_shape=tuple(jax.ShapeDtypeStruct(o.shape, o.dtype) for o in (layer_out, state_next, value_tail, maps_tail)),
        in_specs=[pl.BlockSpec(memory_space=pltpu.VMEM)] * 4,
        out_specs=(pl.BlockSpec(memory_space=pltpu.HBM),) * 4,
        scratch_shapes=[dma((4,))],
        compiler_params=pltpu.CompilerParams(vmem_limit_bytes=8 * 2**20),
        name="hand_over",
    )(layer_out, state_next, value_tail, maps_tail)
    return (
        layer_out,
        state_next.reshape(24, 1, 64, 128),
        jnp.transpose(value_tail, (1, 0, 2)),
        jnp.transpose(maps_tail, (1, 0, 2)),
    )


def solution(mesh):
    rows = ("dp", "tp")
    in_specs = (
        P(rows, "kv"),
        P(),
        P(None, "kv"),
        P(None, "kv"),
        P(None, "kv"),
        P(),
        P(None, "kv"),
        P(None, "kv"),
        P(rows, None, "kv"),
        P(rows, None, "kv"),
        P("kv"),
        P("kv"),
        P("kv"),
        P("kv"),
        P(rows, "kv", None, None),
        P("kv", None),
        P(),
        P(None, "kv"),
        P("kv", None),
    )
    out_specs = (
        P(rows, "kv"),
        P(rows, "kv", None, None),
        P(rows, None, "kv"),
        P(rows, None, "kv"),
    )
    return jax.shard_map(local, mesh=mesh, in_specs=in_specs, out_specs=out_specs, check_vma=False)
```
